32 devices in a mesh: ep: 4 (over y, x), tp: 8 (over z, core).
Axes of the slice: x: 2, y: 2, z: 4, core: 2. Of those that a mesh axis runs over, the one named last changes fastest.
Arguments:
- queries: bfloat16 [2, 1024, 4096], P(None, 'tp', 'ep'), may hold values from -6 to 6
- key_vectors: bfloat16 [2, 1024, 4096], P(None, 'tp', 'ep'), may hold values from -6 to 6
- value_vectors: bfloat16 [2, 1024, 4096], P(None, 'tp', 'ep'), may hold values from -12 to 12
- cumulative_gate: float32 [2, 16, 4096], P(None, 'tp'), may hold values from -4096 to 0, as said below
- expert_input: bfloat16 [4096, 2048], P(('ep', 'tp')), may hold values from -6 to 6
- norm_gain: float32 [2048], replicated, may hold values from 0.1 to 1.9
- group_choice: int32 [4096], P(('ep', 'tp')), may hold values from 0 to 3, as said below
- group_weight: float32 [4096], P(('ep', 'tp')), may hold values from 0.3 to 1
- expert_logits: float32 [4096, 2], P(('ep', 'tp')), may hold values from -6 to 6
- gate_weight: bfloat16 [8, 2048, 2048], P('ep', 'tp'), may hold values from -0.125 to 0.125
- up_weight: bfloat16 [8, 2048, 2048], P('ep', 'tp'), may hold values from -0.125 to 0.125
- down_weight: bfloat16 [8, 2048, 2048], P('ep', 'tp'), may hold values from -0.25 to 0.25
Outputs:
- attention: bfloat16 [2, 1024, 4096], P(None, 'tp', 'ep')
- expert_output: bfloat16 [4096, 2048], P(('ep', 'tp'))
The draws below stay inside these ranges and needn't reach their ends.
Inputs may be any that keep to these rules, and one draw needn't show every extreme that they name: `cumulative_gate`: each row is non-increasing along positions. `group_choice`: in each aligned block of 128 rows (the rows of one device) no group is named more than 40 times, and one group is named exactly 40 times in every block.
All inputs are finite; a program needn't handle non-finite values.
Results may differ from the reference program's by a relative error of at most 0.017.
Values may be sent and summed in bfloat16 or wider, within the bound.
No kernel may reach another device: no remote copies, remote signals or barrier semaphores. Data moves between devices by JAX's collectives and lax.ppermute only.
A program may use at most 128 MiB of HBM per device.

```python
import math
import jax
import jax.numpy as jnp
from jax import lax

D = 2048
HEADS = 16
HEAD = 64
HD = 1024
FE = 2048
EPG = 2
STRAND_TOTAL = 2
SEG = 1024
STRAND_SPAN = 4096
TOK_DEV = 128
MOE_TOKENS = 4096
GROUPS = 4
EXPERTS = 8
CAP = 40
N_TP = 8


def draw_queries(key, part):
    rows = jnp.clip(1.6 * jax.random.normal(jax.random.fold_in(key, 11), (STRAND_TOTAL, STRAND_SPAN, HD), jnp.float32), -6.0, 6.0)
    return jnp.transpose(rows, (0, 2, 1)).astype(jnp.bfloat16)


def draw_key_vectors(key, part):
    rows = jnp.clip(1.6 * jax.random.normal(jax.random.fold_in(key, 12), (STRAND_TOTAL, STRAND_SPAN, HD), jnp.float32), -6.0, 6.0)
    return jnp.transpose(rows, (0, 2, 1)).astype(jnp.bfloat16)


def draw_cumulative_gate(key, part):
    order = jax.random.permutation(jax.random.fold_in(key, 21), HEADS).astype(jnp.int32)
    fast_span = jnp.exp(jax.random.uniform(jax.random.fold_in(key, 23), (STRAND_TOTAL, HEADS), jnp.float32, math.log(30.0), math.log(100.0)))
    slow = order[None, :] < HEADS // 2
    slow_total = jnp.exp(jax.random.uniform(jax.random.fold_in(key, 22), (STRAND_TOTAL, HEADS), jnp.float32, math.log(0.25), math.log(0.8)))
    rate = jnp.where(slow, slow_total / STRAND_SPAN, 1.0 / fast_span)
    block_factor = jnp.exp(jax.random.uniform(jax.random.fold_in(key, 24), (STRAND_TOTAL, 1, STRAND_SPAN // SEG), jnp.float32, math.log(0.5), math.log(2.0)))
    block_factor = jnp.repeat(block_factor, SEG, axis=2)
    jitter = jax.random.uniform(jax.random.fold_in(key, 25), (STRAND_TOTAL, HEADS, STRAND_SPAN), jnp.float32, 0.1, 1.9)
    pass_tally = -rate[:, :, None] * block_factor * jitter
    stretch_shift = jax.random.randint(jax.random.fold_in(key, 26), (STRAND_TOTAL, 2), 1, STRAND_SPAN).astype(jnp.int32)
    stretch_width = jax.random.uniform(jax.random.fold_in(key, 27), (STRAND_TOTAL, 2), jnp.float32, 0.22, 0.69)
    strand_number = jnp.arange(STRAND_TOTAL, dtype=jnp.int32)[:, None]
    stretch_table = jnp.zeros((STRAND_TOTAL, STRAND_SPAN), jnp.float32).at[strand_number, stretch_shift].add(stretch_width)
    pass_tally = pass_tally - stretch_table[:, None, :]
    return jnp.cumsum(pass_tally, axis=2).astype(jnp.float32)


def draw_group_choice(key, part):
    block_total = MOE_TOKENS // TOK_DEV
    pool_size = GROUPS * CAP
    full_group = jax.random.randint(jax.random.fold_in(key, 31), (), 0, GROUPS).astype(jnp.int32)
    owner = (jnp.arange(pool_size, dtype=jnp.int32) // CAP).astype(jnp.int32)

    def one_block(block_index):
        block_key = jax.random.fold_in(key, 1000 + block_index)
        ranked = jax.random.permutation(jax.random.fold_in(block_key, 1), pool_size).astype(jnp.int32)
        priority = jnp.where(owner == full_group, ranked - pool_size, ranked)
        picked = owner[jnp.argsort(priority)[:TOK_DEV]]
        shuffle = jax.random.permutation(jax.random.fold_in(block_key, 2), TOK_DEV)
        return picked[shuffle]
    return jax.vmap(one_block)(jnp.arange(block_total, dtype=jnp.int32)).reshape(MOE_TOKENS).astype(jnp.int32)


def steps_of(stream_key, extent, pieces, smallest, high):
    gain, own = 1.0, jax.random.fold_in(stream_key, 6)
    for dim, blocks in pieces:
        draws = jnp.exp(jax.random.uniform(jax.random.fold_in(own, dim), (blocks,), jnp.float32, smallest / len(pieces), high / len(pieces)))
        gain = gain * jnp.repeat(draws, extent[dim] // blocks).reshape([-1 if axis == dim else 1 for axis in range(len(extent))])
    return gain


def gaussian(rng, dims, scale, most, shards=(), kind=jnp.bfloat16):
    factor_of = steps_of(rng, dims, shards, -0.22, 0.18) if shards else 1.0
    drawn = jax.random.normal(rng, dims, jnp.float32) * scale * factor_of
    return jnp.minimum(jnp.maximum(drawn, -most), most).astype(kind)


def setup_inputs(seed: int = 0) -> dict:
    streams_of = jax.random.split(jax.random.key(seed), 13)
    queries = draw_queries(jax.random.fold_in(streams_of[12], 71), 0)
    key_vectors = draw_key_vectors(jax.random.fold_in(streams_of[12], 71), 0)
    value_vectors = gaussian(streams_of[2], (STRAND_TOTAL, HD, STRAND_SPAN), 2.0, 12.0, ((1, 8), (2, 4)))
    cumulative_gate = draw_cumulative_gate(jax.random.fold_in(streams_of[12], 71), 0)
    expert_input = gaussian(streams_of[4], (MOE_TOKENS, D), 1.0, 6.0, ((0, 32),))
    norm_gain = jnp.clip(1.0 + 0.18 * jax.random.normal(streams_of[5], (D,), jnp.float32), 0.1, 1.9)
    group_choice = draw_group_choice(jax.random.fold_in(streams_of[12], 71), 0)
    group_weight = jnp.clip(jnp.exp(math.log(1.0) - 1.2039728 * jax.random.uniform(streams_of[7], (MOE_TOKENS,), jnp.float32) ** steps_of(streams_of[7], (MOE_TOKENS,), ((0, 32),), -0.2, 0.2)), 0.3, 1.0)
    expert_logits = gaussian(streams_of[8], (MOE_TOKENS, EPG), 1.5, 6.0, ((0, 32),), jnp.float32)
    gate_weight = gaussian(streams_of[9], (EXPERTS, FE, D), D ** -0.5, 0.125, ((0, 4), (1, 8)))
    up_weight = gaussian(streams_of[10], (EXPERTS, FE, D), D ** -0.5, 0.125, ((0, 4), (1, 8)))
    down_weight = gaussian(streams_of[11], (EXPERTS, FE, D), (FE // 4) ** -0.5, 0.25, ((0, 4), (1, 8)))
    return {"queries": queries, "key_vectors": key_vectors, "value_vectors": value_vectors, "cumulative_gate": cumulative_gate, "expert_input": expert_input, "norm_gain": norm_gain, "group_choice": group_choice, "group_weight": group_weight, "expert_logits": expert_logits, "gate_weight": gate_weight, "up_weight": up_weight, "down_weight": down_weight}


neg_fill = -1e+30
norm_eps = 1e-06

def head_attention(queries, key_vectors, value_vectors, cumulative_gate):
    query_rows = jnp.transpose(queries, (0, 2, 1))
    key_rows = jnp.transpose(key_vectors, (0, 2, 1))
    value_rows = jnp.transpose(value_vectors, (0, 2, 1))
    block_len = min(512, STRAND_SPAN)
    block_count = STRAND_SPAN // block_len
    score_scale = 1.0 / math.sqrt(HEAD)
    zero_index = jnp.zeros((), jnp.int32)
    key_positions = jnp.arange(STRAND_SPAN, dtype=jnp.int32)

    def one_pair(pair_index):
        strand_number = (pair_index // HEADS).astype(jnp.int32)
        head_index = (pair_index % HEADS).astype(jnp.int32)
        column = (head_index * HEAD).astype(jnp.int32)
        query_head = lax.dynamic_slice(query_rows, (strand_number, zero_index, column), (1, STRAND_SPAN, HEAD))[0]
        key_head = lax.dynamic_slice(key_rows, (strand_number, zero_index, column), (1, STRAND_SPAN, HEAD))[0]
        value_head = lax.dynamic_slice(value_rows, (strand_number, zero_index, column), (1, STRAND_SPAN, HEAD))[0]
        gate_head = lax.dynamic_slice(cumulative_gate, (strand_number, head_index, zero_index), (1, 1, STRAND_SPAN))[0, 0]

        def one_block(block_index):
            block_start = (block_index * block_len).astype(jnp.int32)
            query_block = lax.dynamic_slice_in_dim(query_head, block_start, block_len, 0)
            query_gate = lax.dynamic_slice_in_dim(gate_head, block_start, block_len, 0)
            scores = jnp.dot(query_block, key_head.T, preferred_element_type=jnp.float32) * score_scale
            scores = scores + (query_gate[:, None] - gate_head[None, :])
            query_positions = block_start + jnp.arange(block_len, dtype=jnp.int32)
            allowed = key_positions[None, :] <= query_positions[:, None]
            scores = jnp.where(allowed, scores, neg_fill)
            peak = lax.optimization_barrier(jnp.max(scores, axis=1, keepdims=True))
            expo = jnp.where(allowed, jnp.exp(scores - peak), 0.0)
            total = lax.optimization_barrier(jnp.sum(expo, axis=1, keepdims=True))
            mixed = jnp.dot(expo.astype(jnp.bfloat16), value_head, preferred_element_type=jnp.float32) / total
            return mixed.astype(jnp.bfloat16)
        return lax.map(one_block, jnp.arange(block_count, dtype=jnp.int32)).reshape(STRAND_SPAN, HEAD)
    heads_out = lax.map(one_pair, jnp.arange(STRAND_TOTAL * HEADS, dtype=jnp.int32))
    heads_out = heads_out.reshape(STRAND_TOTAL, HEADS, STRAND_SPAN, HEAD)
    return jnp.transpose(heads_out, (0, 1, 3, 2)).reshape(STRAND_TOTAL, HD, STRAND_SPAN)

def expert_mixture(expert_input, norm_gain, group_choice, group_weight, expert_logits, gate_weight, up_weight, down_weight):
    token_float = expert_input.astype(jnp.float32)
    normed = (token_float * lax.rsqrt(lax.optimization_barrier(jnp.mean(token_float * token_float, axis=1, keepdims=True)) + norm_eps) * norm_gain).astype(jnp.bfloat16)
    routing = (group_weight[:, None] * jax.nn.softmax(expert_logits, axis=1)).astype(jnp.bfloat16)
    block_total = MOE_TOKENS // TOK_DEV
    chosen = group_choice.reshape(block_total, TOK_DEV)
    member = (chosen[:, :, None] == jnp.arange(GROUPS, dtype=jnp.int32)[None, None, :]).astype(jnp.int32)
    before = jnp.cumsum(member, axis=1) - member
    slot_index = lax.optimization_barrier(jnp.sum(before * member, axis=2))
    block_ids = jnp.arange(block_total, dtype=jnp.int32)[:, None]
    flat_slot = ((chosen * block_total + block_ids) * CAP + slot_index).reshape(MOE_TOKENS).astype(jnp.int32)
    row_total = block_total * CAP
    row_buffer = jnp.zeros((GROUPS * row_total, D), jnp.bfloat16).at[flat_slot].set(normed).reshape(GROUPS, row_total, D)
    route_buffer = jnp.zeros((GROUPS * row_total, EPG), jnp.bfloat16).at[flat_slot].set(routing).reshape(GROUPS, row_total, EPG)
    hidden_width = FE // N_TP

    def one_group(group_index):
        group_rows = lax.optimization_barrier(row_buffer[group_index]).astype(jnp.float32)
        group_route = lax.optimization_barrier(route_buffer[group_index]).astype(jnp.float32)
        first_expert = (group_index * EPG).astype(jnp.int32)
        gate_block = lax.dynamic_slice_in_dim(gate_weight, first_expert, EPG, 0).astype(jnp.float32)
        up_block = lax.dynamic_slice_in_dim(up_weight, first_expert, EPG, 0).astype(jnp.float32)
        down_block = lax.dynamic_slice_in_dim(down_weight, first_expert, EPG, 0).astype(jnp.float32)
        gate_act = jnp.einsum('rd,efd->ref', group_rows, gate_block)
        up_act = jnp.einsum('rd,efd->ref', group_rows, up_block)
        hidden = (jax.nn.silu(gate_act) * up_act * group_route[:, :, None]).astype(jnp.bfloat16)
        hidden = lax.optimization_barrier(hidden).astype(jnp.float32).reshape(row_total, EPG, N_TP, hidden_width)
        partial_sums = jnp.einsum('rejf,ejfd->rjd', hidden, down_block.reshape(EPG, N_TP, hidden_width, D))
        partial_sums = lax.optimization_barrier(partial_sums.astype(jnp.bfloat16)).astype(jnp.float32)
        return lax.optimization_barrier(jnp.sum(partial_sums, axis=1)).astype(jnp.bfloat16)
    group_out = lax.map(one_group, jnp.arange(GROUPS, dtype=jnp.int32))
    return group_out.reshape(GROUPS * row_total, D)[flat_slot]

def reference(queries, key_vectors, value_vectors, cumulative_gate, expert_input, norm_gain, group_choice, group_weight, expert_logits, gate_weight, up_weight, down_weight):
    attention = head_attention(queries, key_vectors, value_vectors, cumulative_gate)
    expert_output = expert_mixture(expert_input, norm_gain, group_choice, group_weight, expert_logits, gate_weight, up_weight, down_weight)
    return (attention, expert_output)
```

```python
from functools import partial
import math

import jax
import jax.numpy as jnp
from jax import lax
from jax.experimental import pallas as pl
from jax.experimental.pallas import tpu as pltpu
from jax.sharding import PartitionSpec as P

neg_fill = -1e30
norm_eps = 1e-06


def partner(x, axis, distance):
    return lax.ppermute(x, axis, [(i, i ^ 1 << distance) for i in range(lax.axis_size(axis))])


def spread(x, descending):
    bits = list(range(lax.axis_size("ep").bit_length() - 1))
    if descending:
        bits = bits[::-1]
    stages, offsets = [x[None]], [[0]]
    for bit_index in bits:
        everything = jnp.concatenate(stages, axis=0) if len(stages) > 1 else stages[0]
        held = [o for group in offsets for o in group]
        stages.append(partner(everything, "ep", bit_index))
        offsets.append([o ^ (1 << bit_index) for o in held])
    where = {}
    for stage_index, group in enumerate(offsets):
        for place, offset in enumerate(group):
            where[offset] = (stage_index, place)
    return stages, where


def flash_body(
    flags, q_ref, g_ref, *rest, key_where, value_where, key_count, value_count, head_dim, tile, scale
):
    k_refs = rest[:key_count]
    v_refs = rest[key_count : key_count + value_count]
    o_ref, m_ref, acc_ref = rest[key_count + value_count :]
    seg_len = q_ref.shape[-1]
    tiles = seg_len // tile
    extra = g_ref.shape[-2]
    to_log2 = scale * math.log2(math.e)
    row = lax.broadcasted_iota(jnp.int32, (extra, tile), 0)
    ones_q = jnp.where(row < 3, 1.0, 0.0).astype(jnp.bfloat16)

    def key_rows(offset, start, length):
        stage, place = key_where[offset]
        keys = k_refs[stage][place, 0, :, start : start + length]
        return jnp.concatenate([keys, g_ref[offset, 0, 0, :, start : start + length]], axis=0)

    def value_rows(offset, start, length):
        stage, place = value_where[offset]
        values = v_refs[stage][place, 0, :, start : start + length]
        return jnp.concatenate([values, jnp.ones((extra, length), jnp.bfloat16)], axis=0)

    def step(state, queries, offset, start, length, diagonal):
        peak_old, acc_old = state
        scores = lax.dot_general(
            key_rows(offset, start, length),
            queries,
            (((0,), (0,)), ((), ())),
            preferred_element_type=jnp.float32,
        )
        scores = scores * to_log2
        if diagonal:
            key_pos = lax.broadcasted_iota(jnp.int32, scores.shape, 0)
            query_pos = lax.broadcasted_iota(jnp.int32, scores.shape, 1)
            scores = jnp.where(key_pos <= query_pos, scores, neg_fill)
        peak_new = jnp.maximum(peak_old, jnp.max(scores, axis=0, keepdims=True))
        weights = jnp.exp2(scores - peak_new).astype(jnp.bfloat16)
        shrink = jnp.exp2(peak_old - peak_new)
        acc_new = acc_old * shrink + jnp.dot(
            value_rows(offset, start, length), weights, preferred_element_type=jnp.float32
        )
        return peak_new, acc_new

    def query_rows(start):
        return jnp.concatenate([q_ref[0, :, pl.ds(start, tile)], ones_q], axis=0)

    for index in range(tiles):
        start = index * tile
        queries = query_rows(start)
        state = (
            jnp.full((1, tile), neg_fill, jnp.float32),
            jnp.zeros((head_dim + extra, tile), jnp.float32),
        )
        state = step(state, queries, 0, start, tile, True)
        if index:
            state = step(state, queries, 0, 0, start, False)
        m_ref[:, start : start + tile] = state[0]
        acc_ref[:, start : start + tile] = state[1]

    for offset in range(1, len(key_where)):

        @pl.when(flags[offset] > 0)
        def _(offset=offset):
            @pl.loop(0, tiles)
            def _(index):
                start = pl.multiple_of(index * tile, tile)
                columns = pl.ds(start, tile)
                state = (m_ref[:, columns], acc_ref[:, columns])
                state = step(state, query_rows(start), offset, 0, seg_len, False)
                m_ref[:, columns] = state[0]
                acc_ref[:, columns] = state[1]

    o_ref[0] = (acc_ref[:head_dim, :] / acc_ref[head_dim : head_dim + 1, :]).astype(jnp.bfloat16)


def three_parts(x):
    high = lax.reduce_precision(x, 8, 7)
    rest = x - high
    middle = lax.reduce_precision(rest, 8, 7)
    low = rest - middle
    return jnp.stack([high, middle, low], axis=-2)


def attend(queries, key_stages, key_where, value_stages, value_where, cumulative_gate):
    seq_count, feat_width, seg_len = queries.shape
    heads_here = cumulative_gate.shape[1]
    head_dim = feat_width // heads_here
    ep_size = lax.axis_size("ep")
    ep_rank = lax.axis_index("ep")
    extra = 16
    tile = math.gcd(seg_len, 256)
    anchor = lax.dynamic_slice_in_dim(cumulative_gate, ep_rank * seg_len, 1, 2)
    shifted = (anchor - cumulative_gate) * math.sqrt(head_dim)
    parts = three_parts(shifted).astype(jnp.bfloat16)
    parts = jnp.pad(parts, ((0, 0), (0, 0), (0, extra - 3), (0, 0)))
    gates = jnp.stack(
        [
            lax.dynamic_slice_in_dim(parts, (ep_rank ^ offset) * seg_len, seg_len, 3)
            for offset in range(ep_size)
        ]
    )
    flags = ((ep_rank ^ jnp.arange(ep_size, dtype=jnp.int32)) < ep_rank).astype(jnp.int32)

    def piece_spec(x):
        return pl.BlockSpec((x.shape[0], 1, head_dim, seg_len), lambda s, h, f: (0, s, h, 0))

    one = pl.BlockSpec((1, head_dim, seg_len), lambda s, h, f: (s, h, 0))
    gate_spec = pl.BlockSpec((ep_size, 1, 1, extra, seg_len), lambda s, h, f: (0, s, h, 0, 0))
    pairs = seq_count * heads_here * seg_len * seg_len * ep_size
    return pl.pallas_call(
        partial(
            flash_body,
            key_where=key_where,
            value_where=value_where,
            key_count=len(key_stages),
            value_count=len(value_stages),
            head_dim=head_dim,
            tile=tile,
            scale=1.0 / math.sqrt(head_dim),
        ),
        out_shape=jax.ShapeDtypeStruct(queries.shape, jnp.bfloat16),
        grid_spec=pltpu.PrefetchScalarGridSpec(
            num_scalar_prefetch=1,
            grid=(seq_count, heads_here),
            in_specs=[one, gate_spec] + [piece_spec(x) for x in key_stages + value_stages],
            out_specs=one,
            scratch_shapes=[
                pltpu.VMEM((1, seg_len), jnp.float32),
                pltpu.VMEM((head_dim + extra, seg_len), jnp.float32),
            ],
        ),
        cost_estimate=pl.CostEstimate(
            flops=16 * pairs * head_dim, transcendentals=pairs, bytes_accessed=8 * queries.size * ep_size
        ),
        name="flash",
    )(flags, queries, gates, *key_stages, *value_stages)


def swap_blocks(x, dim, capacity):
    blocks = [
        lax.slice_in_dim(x, j * capacity, (j + 1) * capacity, axis=dim)
        for j in range(x.shape[dim] // capacity)
    ]
    size = lax.axis_size("ep")
    swapped = [
        lax.ppermute(block, "ep", [(i, i ^ j) for i in range(size)]) if j else block
        for j, block in enumerate(blocks)
    ]
    return jnp.concatenate(swapped, axis=dim)


def expert_hidden(row_block, route_block, gate_weight, up_weight):
    gate_act = jnp.einsum("rd,efd->ref", row_block, gate_weight, preferred_element_type=jnp.float32)
    up_act = jnp.einsum("rd,efd->ref", row_block, up_weight, preferred_element_type=jnp.float32)
    return (jax.nn.silu(gate_act) * up_act * route_block.astype(jnp.float32)[:, :, None]).astype(
        jnp.bfloat16
    )


def mixture(
    expert_input,
    norm_gain,
    group_choice,
    group_weight,
    expert_logits,
    gate_weight,
    up_weight,
    down_weight,
):
    tok_rows, model_dim = expert_input.shape
    group_size = gate_weight.shape[0]
    ep_size = lax.axis_size("ep")
    capacity = 5 * tok_rows // (4 * ep_size)
    token_float = expert_input.astype(jnp.float32)
    normed = (
        token_float
        * lax.rsqrt(jnp.mean(token_float * token_float, axis=1, keepdims=True) + norm_eps)
        * norm_gain
    ).astype(jnp.bfloat16)
    routing = (group_weight[:, None] * jax.nn.softmax(expert_logits, axis=1)).astype(jnp.bfloat16)
    ep_rank = lax.axis_index("ep")
    member = (group_choice[:, None] == jnp.arange(ep_size, dtype=jnp.int32)[None, :]).astype(
        jnp.int32
    )
    before = jnp.cumsum(member, axis=0) - member
    slot_index = jnp.sum(before * member, axis=1)
    flat_slot = (group_choice ^ ep_rank) * capacity + slot_index
    places = (
        flat_slot[None, :] == jnp.arange(ep_size * capacity, dtype=jnp.int32)[:, None]
    ).astype(jnp.bfloat16)
    outgoing = jnp.dot(places, normed, preferred_element_type=jnp.float32).astype(jnp.bfloat16)
    send_route = lax.dot_general(
        routing, places, (((0,), (1,)), ((), ())), preferred_element_type=jnp.float32
    ).astype(jnp.bfloat16)
    local_rows = swap_blocks(outgoing, 0, capacity)
    local_route = swap_blocks(send_route, 1, capacity)
    gathered_rows = lax.all_gather(local_rows, "tp", axis=0, tiled=True)
    gathered_route = local_route
    for bit_index in range(lax.axis_size("tp").bit_length() - 1):
        other = partner(gathered_route, "tp", bit_index)
        upper = ((lax.axis_index("tp") >> bit_index) & 1) == 1
        gathered_route = jnp.concatenate(
            [
                jnp.where(upper, other, gathered_route),
                jnp.where(upper, gathered_route, other),
            ],
            axis=1,
        )
    gathered_route = gathered_route.T
    hidden = expert_hidden(gathered_rows, gathered_route, gate_weight, up_weight)
    partial_sums = jnp.einsum(
        "ref,efd->rd", hidden, down_weight, preferred_element_type=jnp.float32
    ).astype(jnp.bfloat16)

    def finish(partial_sums):
        summed = lax.psum_scatter(partial_sums, "tp", scatter_dimension=0, tiled=True)
        returned_flat = swap_blocks(summed, 0, capacity)
        return jnp.einsum(
            "pt,pd->td", places, returned_flat, preferred_element_type=jnp.float32
        ).astype(jnp.bfloat16)

    return local_rows, partial_sums, finish


def local(
    queries,
    key_vectors,
    value_vectors,
    cumulative_gate,
    expert_input,
    norm_gain,
    group_choice,
    group_weight,
    expert_logits,
    gate_weight,
    up_weight,
    down_weight,
):
    local_rows, partial_sums, finish = mixture(
        expert_input,
        norm_gain,
        group_choice,
        group_weight,
        expert_logits,
        gate_weight,
        up_weight,
        down_weight,
    )
    key_vectors, value_vectors, _ = lax.optimization_barrier(
        (key_vectors, value_vectors, local_rows)
    )
    key_stages, key_where = spread(key_vectors, False)
    value_stages, value_where = spread(value_vectors, True)
    queries, partial_sums = lax.optimization_barrier((queries, partial_sums))
    attention = attend(
        queries, key_stages, key_where, value_stages, value_where, cumulative_gate
    )
    return (attention, finish(partial_sums))


def solution(mesh):
    return jax.shard_map(
        local,
        mesh=mesh,
        in_specs=(
            P(None, "tp", "ep"),
            P(None, "tp", "ep"),
            P(None, "tp", "ep"),
            P(None, "tp", None),
            P(("ep", "tp"), None),
            P(),
            P(("ep", "tp")),
            P(("ep", "tp")),
            P(("ep", "tp"), None),
            P("ep", "tp", None),
            P("ep", "tp", None),
            P("ep", "tp", None),
        ),
        out_specs=(P(None, "tp", "ep"), P(("ep", "tp"), None)),
        check_vma=False,
    )
```

```python
from functools import partial
import math

import jax
import jax.numpy as jnp
from jax import lax
from jax.experimental import pallas as pl
from jax.experimental.pallas import tpu as pltpu
from jax.sharding import PartitionSpec as P

neg_fill = -1e30
norm_eps = 1e-06
query_tile = 1024
key_span = 256
diagonal_span = 256


def partner(x, axis, distance):
    return lax.ppermute(x, axis, [(i, i ^ 1 << distance) for i in range(lax.axis_size(axis))])


def spread_plan(descending):
    bits = list(range(lax.axis_size("ep").bit_length() - 1))
    if descending:
        bits = bits[::-1]
    moves, held = [], [0]
    for bit_index in bits:
        moves += [(offset, bit_index) for offset in held]
        held = held + [offset ^ (1 << bit_index) for offset in held]
    return moves


def flash_body(
    flags, q_ref, g_ref, *rest, piece_count, head_dim, scale
):
    k_refs = rest[:piece_count]
    v_refs = rest[piece_count : 2 * piece_count]
    o_ref, m_ref, acc_ref = rest[2 * piece_count :]
    seg_len = q_ref.shape[-1]
    tile = math.gcd(seg_len, query_tile)
    span = math.gcd(seg_len, key_span)
    first = math.gcd(seg_len, diagonal_span)
    extra = g_ref.shape[-2]
    to_log2 = scale * math.log2(math.e)

    def step(state, queries, offset, start, length, diagonal):
        peak_old, acc_old = state
        keys = jnp.concatenate(
            [k_refs[offset][0, :, start : start + length], g_ref[offset, 0, 0, :, start : start + length]],
            axis=0,
        )
        values = jnp.concatenate(
            [v_refs[offset][0, :, start : start + length], jnp.ones((extra, length), jnp.bfloat16)],
            axis=0,
        )
        scores = lax.dot_general(
            keys, queries, (((0,), (0,)), ((), ())), preferred_element_type=jnp.float32
        )
        scores = scores * to_log2
        if diagonal:
            key_pos = lax.broadcasted_iota(jnp.int32, scores.shape, 0)
            query_pos = lax.broadcasted_iota(jnp.int32, scores.shape, 1)
            scores = jnp.where(key_pos <= query_pos, scores, neg_fill)
        peak_new = jnp.maximum(peak_old, jnp.max(scores, axis=0, keepdims=True))
        weights = jnp.exp2(scores - peak_new).astype(jnp.bfloat16)
        shrink = jnp.exp2(peak_old - peak_new)
        acc_new = acc_old * shrink + jnp.dot(values, weights, preferred_element_type=jnp.float32)
        return peak_new, acc_new

    def query_rows(start, width):
        row = lax.broadcasted_iota(jnp.int32, (extra, width), 0)
        ones_q = jnp.where(row < 3, 1.0, 0.0).astype(jnp.bfloat16)
        return jnp.concatenate([q_ref[0, :, start : start + width], ones_q], axis=0)

    m_ref[...] = jnp.full(m_ref.shape, neg_fill, jnp.float32)
    acc_ref[...] = jnp.zeros(acc_ref.shape, jnp.float32)
    for start in range(0, seg_len, first):
        state = (m_ref[:, start:], acc_ref[:, start:])
        state = step(state, query_rows(start, seg_len - start), 0, start, first, True)
        m_ref[:, start:] = state[0]
        acc_ref[:, start:] = state[1]

    for offset in range(1, piece_count):

        @pl.when(flags[offset] > 0)
        def _(offset=offset):
            for start in range(0, seg_len, tile):
                columns = slice(start, start + tile)
                state = (m_ref[:, columns], acc_ref[:, columns])
                queries = query_rows(start, tile)
                for begin in range(0, seg_len, span):
                    state = step(state, queries, offset, begin, span, False)
                m_ref[:, columns] = state[0]
                acc_ref[:, columns] = state[1]

    o_ref[0] = (acc_ref[:head_dim, :] / acc_ref[head_dim : head_dim + 1, :]).astype(jnp.bfloat16)


def three_parts(x):
    high = lax.reduce_precision(x, 8, 7)
    rest = x - high
    middle = lax.reduce_precision(rest, 8, 7)
    low = rest - middle
    return jnp.stack([high, middle, low], axis=-2)


def attend_gates(queries, cumulative_gate):
    _, feat_width, seg_len = queries.shape
    head_dim = feat_width // cumulative_gate.shape[1]
    ep_size = lax.axis_size("ep")
    ep_rank = lax.axis_index("ep")
    extra = 16
    anchor = lax.dynamic_slice_in_dim(cumulative_gate, ep_rank * seg_len, 1, 2)
    shifted = (anchor - cumulative_gate) * math.sqrt(head_dim)
    parts = three_parts(shifted).astype(jnp.bfloat16)
    parts = jnp.pad(parts, ((0, 0), (0, 0), (0, extra - 3), (0, 0)))
    gates = jnp.stack(
        [
            lax.dynamic_slice_in_dim(parts, (ep_rank ^ offset) * seg_len, seg_len, 3)
            for offset in range(ep_size)
        ]
    )
    return gates


def attend(sequence, head, queries, keys, values, gates):
    _, feat_width, seg_len = queries.shape
    ep_size, _, heads_here, extra, _ = gates.shape
    head_dim = feat_width // heads_here
    ep_rank = lax.axis_index("ep")
    flags = ((ep_rank ^ jnp.arange(ep_size, dtype=jnp.int32)) < ep_rank).astype(jnp.int32)
    one = pl.BlockSpec((1, head_dim, seg_len), lambda i, f: (sequence, head, 0))
    gate_spec = pl.BlockSpec(
        (ep_size, 1, 1, extra, seg_len), lambda i, f: (0, sequence, head, 0, 0)
    )
    pairs = seg_len * seg_len * ep_size
    return pl.pallas_call(
        partial(
            flash_body, piece_count=ep_size, head_dim=head_dim, scale=1.0 / math.sqrt(head_dim)
        ),
        out_shape=jax.ShapeDtypeStruct((1, head_dim, seg_len), jnp.bfloat16),
        grid_spec=pltpu.PrefetchScalarGridSpec(
            num_scalar_prefetch=1,
            grid=(1,),
            in_specs=[one, gate_spec] + [one] * (2 * ep_size),
            out_specs=pl.BlockSpec((1, head_dim, seg_len), lambda i, f: (0, 0, 0)),
            scratch_shapes=[
                pltpu.VMEM((1, seg_len), jnp.float32),
                pltpu.VMEM((head_dim + extra, seg_len), jnp.float32),
            ],
        ),
        cost_estimate=pl.CostEstimate(
            flops=16 * pairs * head_dim, transcendentals=pairs, bytes_accessed=16 * queries.size
        ),
        name="flash",
    )(flags, queries, gates, *keys, *values)


def swap_blocks(x, dim, capacity):
    blocks = [
        lax.slice_in_dim(x, j * capacity, (j + 1) * capacity, axis=dim)
        for j in range(x.shape[dim] // capacity)
    ]
    size = lax.axis_size("ep")
    swapped = [
        lax.ppermute(block, "ep", [(i, i ^ j) for i in range(size)]) if j else block
        for j, block in enumerate(blocks)
    ]
    return jnp.concatenate(swapped, axis=dim)


def expert_hidden(row_block, route_block, gate_weight, up_weight):
    gate_act = jnp.einsum("rd,efd->ref", row_block, gate_weight, preferred_element_type=jnp.float32)
    up_act = jnp.einsum("rd,efd->ref", row_block, up_weight, preferred_element_type=jnp.float32)
    return (jax.nn.silu(gate_act) * up_act * route_block.astype(jnp.float32)[:, :, None]).astype(
        jnp.bfloat16
    )


def dispatch(expert_input, norm_gain, group_choice, group_weight, expert_logits):
    tok_rows = expert_input.shape[0]
    ep_size = lax.axis_size("ep")
    capacity = 5 * tok_rows // (4 * ep_size)
    token_float = expert_input.astype(jnp.float32)
    normed = (
        token_float
        * lax.rsqrt(jnp.mean(token_float * token_float, axis=1, keepdims=True) + norm_eps)
        * norm_gain
    ).astype(jnp.bfloat16)
    routing = (group_weight[:, None] * jax.nn.softmax(expert_logits, axis=1)).astype(jnp.bfloat16)
    ep_rank = lax.axis_index("ep")
    member = (group_choice[:, None] == jnp.arange(ep_size, dtype=jnp.int32)[None, :]).astype(
        jnp.int32
    )
    before = jnp.cumsum(member, axis=0) - member
    slot_index = jnp.sum(before * member, axis=1)
    flat_slot = (group_choice ^ ep_rank) * capacity + slot_index
    places = (
        flat_slot[None, :] == jnp.arange(ep_size * capacity, dtype=jnp.int32)[:, None]
    ).astype(jnp.bfloat16)
    outgoing = jnp.dot(places, normed, preferred_element_type=jnp.float32).astype(jnp.bfloat16)
    send_route = lax.dot_general(
        routing, places, (((0,), (1,)), ((), ())), preferred_element_type=jnp.float32
    ).astype(jnp.bfloat16)
    local_rows = swap_blocks(outgoing, 0, capacity)
    local_route = swap_blocks(send_route, 1, capacity)
    gathered_route = local_route
    for bit_index in range(lax.axis_size("tp").bit_length() - 1):
        other = partner(gathered_route, "tp", bit_index)
        upper = ((lax.axis_index("tp") >> bit_index) & 1) == 1
        gathered_route = jnp.concatenate(
            [
                jnp.where(upper, other, gathered_route),
                jnp.where(upper, gathered_route, other),
            ],
            axis=1,
        )
    return places, local_rows, gathered_route


def experts(local_rows, gathered_route, weights, exchanges, pieces, operand):
    gate_weight, up_weight, down_weight = weights
    arrived = lax.all_gather(local_rows, "tp", axis=0, tiled=True)
    for exchange in exchanges[:-1]:
        arrived = exchange(arrived)
    hidden = expert_hidden(arrived, gathered_route.T, gate_weight, up_weight)
    partial_sums = jnp.einsum(
        "ref,efd->rd", hidden, down_weight, preferred_element_type=jnp.float32
    ).astype(jnp.bfloat16)
    for exchange in exchanges[-1:]:
        partial_sums = exchange(partial_sums)
    operand, partial_sums = lax.optimization_barrier((operand, partial_sums))
    summed = lax.psum_scatter(partial_sums, "tp", scatter_dimension=0, tiled=True)
    attention = [run(operand) for run in pieces]
    attention, summed = lax.optimization_barrier((attention, summed))
    return summed, attention


def local(
    queries,
    key_vectors,
    value_vectors,
    cumulative_gate,
    expert_input,
    norm_gain,
    group_choice,
    group_weight,
    expert_logits,
    gate_weight,
    up_weight,
    down_weight,
):
    places, local_rows, gathered_route = dispatch(
        expert_input, norm_gain, group_choice, group_weight, expert_logits
    )
    key_vectors, value_vectors, _ = lax.optimization_barrier(
        (key_vectors, value_vectors, local_rows)
    )
    size = lax.axis_size("ep")
    keys = {0: key_vectors}
    values = {0: value_vectors}
    gates = attend_gates(queries, cumulative_gate)

    def exchange(arrived, key_move, value_move):
        fresh = []
        for held, (offset, bit_index) in ((keys, key_move), (values, value_move)):
            fresh.append(partner(held[offset], "ep", bit_index))
        arrived, fresh = lax.optimization_barrier((arrived, fresh))
        for held, (offset, bit_index), piece in zip((keys, values), (key_move, value_move), fresh):
            held[offset ^ (1 << bit_index)] = piece
        return arrived

    def run(operand, sequence, head):
        return attend(
            sequence,
            head,
            operand,
            [keys[offset] for offset in range(size)],
            [values[offset] for offset in range(size)],
            gates,
        )

    seq_count, heads_here = cumulative_gate.shape[:2]
    summed, attention = experts(
        local_rows,
        gathered_route,
        (gate_weight, up_weight, down_weight),
        [
            partial(exchange, key_move=key_move, value_move=value_move)
            for key_move, value_move in zip(spread_plan(False), spread_plan(True))
        ],
        [
            partial(run, sequence=sequence, head=head)
            for sequence in range(seq_count)
            for head in range(heads_here)
        ],
        queries,
    )
    returned_flat = swap_blocks(summed, 0, local_rows.shape[0] // lax.axis_size("ep"))
    expert_output = jnp.einsum(
        "pt,pd->td", places, returned_flat, preferred_element_type=jnp.float32
    ).astype(jnp.bfloat16)
    attention = jnp.concatenate(attention, axis=0).reshape(queries.shape)
    return (attention, expert_output)


def solution(mesh):
    return jax.shard_map(
        local,
        mesh=mesh,
        in_specs=(
            P(None, "tp", "ep"),
            P(None, "tp", "ep"),
            P(None, "tp", "ep"),
            P(None, "tp", None),
            P(("ep", "tp"), None),
            P(),
            P(("ep", "tp")),
            P(("ep", "tp")),
            P(("ep", "tp"), None),
            P("ep", "tp", None),
            P("ep", "tp", None),
            P("ep", "tp", None),
        ),
        out_specs=(P(None, "tp", "ep"), P(("ep", "tp"), None)),
        check_vma=False,
    )
```
